32 devices in a mesh: sp: 4 (over y, x), tp: 8 (over z, core).
Axes of the slice: x: 2, y: 2, z: 4, core: 2. Of those that a mesh axis runs over, the one named last changes fastest.
Arguments:
- moe_input: bfloat16 [1024, 4096], P('sp', 'tp'), may hold values from -6 to 6
- out_gate: bfloat16 [1024, 4096], P('sp', 'tp'), may hold values from -6 to 6
- in_gate: bfloat16 [1024, 4096], P('sp', 'tp'), may hold values from -6 to 6
- values: bfloat16 [1024, 4096], P('sp', 'tp'), may hold values from -6 to 6
- conv_taps: float32 [3, 4096], P(None, 'tp'), may hold values from -3 to 3
- out_proj: bfloat16 [4096, 4096], P(None, 'tp'), may hold values from -0.09375 to 0.09375
- route_ids: int32 [1024, 2], P('sp'), may hold values from 0 to 3, all different within a row; in each aligned block of 256 rows (0 to 255, 256 to 511, ...) at most 192 rows name the same one
- route_gates: float32 [1024, 2], P('sp'), may hold values from 0.1 to 0.9
- expert_gate: bfloat16 [4, 4096, 2048], P('sp', None, 'tp'), may hold values from -0.09375 to 0.09375
- expert_up: bfloat16 [4, 4096, 2048], P('sp', None, 'tp'), may hold values from -0.09375 to 0.09375
- expert_down: bfloat16 [4, 2048, 4096], P('sp', 'tp'), may hold values from -0.125 to 0.125
- cotangent: bfloat16 [1024, 4096], P('sp', 'tp'), may hold values from -6 to 6
Outputs:
- grad_out_gate: bfloat16 [1024, 4096], P('sp', 'tp')
- grad_in_gate: bfloat16 [1024, 4096], P('sp', 'tp')
- grad_values: bfloat16 [1024, 4096], P('sp', 'tp')
- grad_out_proj: float32 [4096, 4096], P('sp', 'tp')
- grad_expert_gate: float32 [4, 4096, 2048], P('sp', None, 'tp')
- grad_expert_up: float32 [4, 4096, 2048], P('sp', None, 'tp')
- grad_expert_down: float32 [4, 2048, 4096], P('sp', 'tp')
The draws below stay inside these ranges and needn't reach their ends.
Inputs may be any that keep to these rules, and one draw needn't show every extreme that they name: `route_ids`: the 2 experts of a token differ. In the rows of one device no expert is named by more than 192 assignments, and in some device's rows some expert is named by exactly 192.
All inputs are finite; a program needn't handle non-finite values.
Results may differ from the reference program's by a relative error of at most 0.014.
Values may be sent and summed in bfloat16 or wider, within the bound.
A program may use at most 128 MiB of HBM per device.

```python
import math
import jax
import jax.numpy as jnp
import numpy as np
from jax import lax

D = 4096
C = 4096
F = 2048
TOP = 2
TOK = 256
EXPERTS = 4
CAP = 192
TOKENS = 1024
N_SP = 4


def strengthened(drawn, rng, source, target, blocks, factor):
    def block_of(dim):
        return (jnp.arange(drawn.shape[dim]) // (drawn.shape[dim] // blocks)).reshape((-1,) + (1,) * (drawn.ndim - 1 - dim))

    one_side = jax.random.permutation(rng, blocks)[block_of(target)]
    far = (block_of(target) + blocks // 2) % blocks
    return jnp.where((block_of(source) == one_side) | (block_of(source) == far), factor * drawn, drawn)


def steps_of(stream_key, shape, pieces, low, high):
    gain = 1.0
    for dim, parts in pieces:
        steps = jax.random.uniform(jax.random.fold_in(jax.random.fold_in(stream_key, 6), dim), (parts,), jnp.float32, low / len(pieces), high / len(pieces))
        gain = gain * jnp.repeat(jnp.exp(steps), shape[dim] // parts).reshape((-1,) + (1,) * (len(shape) - 1 - dim))
    return gain


def deal_out(key, own, number, rows, number_of, top, bound, slope):
    order = jax.random.permutation(key, number_of)
    crowded, common = load_shares(number_of, rows * top, bound, slope, True), load_shares(number_of, rows * top, bound, slope, False)
    places = jnp.arange(number_of)

    def named(sizes, turn):
        used = int((sizes > 0).sum())
        fixed = max(1, used // 4)
        moved = fixed + (places - fixed + turn * (used - fixed)) % max(1, number_of - fixed)
        return jnp.zeros((number_of,), jnp.int32).at[order[jnp.where(places < fixed, places, moved)]].set(jnp.asarray(sizes, jnp.int32))

    sizes = jnp.where(number % 4 == 0, named(crowded, number // 4), named(common, number - number // 4 - 1))
    mixed = jax.random.permutation(jax.random.fold_in(own, 3), number_of)
    source_of, receiver = mixed[0:number_of // 2 * 2:2], mixed[1:number_of // 2 * 2:2]
    margin = jnp.minimum(sizes[source_of] - 1, bound - sizes[receiver]) // 2
    margin = jnp.where((source_of == order[0]) | (receiver == order[0]) | (sizes[receiver] == 0), 0, jnp.maximum(margin, 0))
    moved = jax.random.randint(jax.random.fold_in(own, 4), (number_of // 2,), 0, 1 << 20) % (margin + 1)
    sizes = sizes.at[source_of].add(-moved).at[receiver].add(moved)
    items = jnp.searchsorted(jnp.cumsum(sizes), jnp.arange(rows * top), side="right").astype(jnp.int32)
    table = items.reshape(top, rows).T
    table = table[jax.random.permutation(jax.random.fold_in(own, 1), rows)]
    turn = jax.random.randint(jax.random.fold_in(own, 2), (rows, 1), 0, top)
    return jnp.take_along_axis(table, (jnp.arange(top)[None, :] + turn) % top, axis=1)


def load_shares(amount, total, bound, skew, full):
    loads = [(1 << 20) // math.isqrt(standing ** skew) + 1 for standing in range(1, amount + 1)]
    largest = bound if full else min(bound, max(-(-total // amount), total * loads[0] // sum(loads)))
    least = 1 if total - largest >= amount - 1 else 0
    holding, rest = [largest] + [least] * (amount - 1), total - largest - least * (amount - 1)
    while rest > 0:
        free = [i for i in range(1, amount) if holding[i] < largest] or [i for i in range(1, amount) if holding[i] < bound]
        whole, remaining = sum([loads[i] for i in free]), rest
        for i in free:
            addition = min(bound - holding[i], max(1, remaining * loads[i] // whole), rest)
            holding[i] = holding[i] + addition
            rest = rest - addition
    return np.array(holding)


def bell_draw(stream_key, shape, spread, most, cuts=(), kind=jnp.bfloat16):
    entries = spread * jax.random.normal(stream_key, shape, jnp.float32)
    if cuts:
        entries = entries * steps_of(stream_key, shape, cuts, -0.22, 0.18)
    return jnp.clip(entries, -most, most).astype(kind)


def gaussian_with(own_key, shape, scale, bound, split, heavy, kind=jnp.bfloat16):
    result = scale * jax.random.normal(own_key, shape, jnp.float32)
    if split:
        result = result * steps_of(own_key, shape, split, -0.22, 0.18)
    return jnp.clip(strengthened(result, jax.random.fold_in(own_key, 3), *heavy), -bound, bound).astype(kind)


def setup_inputs(seed: int = 0) -> dict:
    key_list = jax.random.split(jax.random.key(seed), 13)
    moe_input = bell_draw(key_list[0], (TOKENS, D), 1.0, 6.0, ((0, 4), (1, 8)))
    out_gate = bell_draw(key_list[1], (TOKENS, C), 1.0, 6.0, ((0, 4), (1, 8)))
    in_gate = bell_draw(key_list[2], (TOKENS, C), 1.0, 6.0, ((0, 4), (1, 8)))
    values = bell_draw(key_list[3], (TOKENS, C), 1.0, 6.0, ((0, 4), (1, 8)))
    conv_taps = bell_draw(key_list[4], (3, C), 0.5, 3.0, ((1, 8),), jnp.float32)
    out_proj = bell_draw(key_list[5], (D, C), C ** -0.5, 0.09375, ((1, 8),))
    route_ids_keys = jax.random.split(jax.random.fold_in(key_list[6], 1), TOKENS // TOK)
    route_ids_turns = jax.random.permutation(jax.random.fold_in(key_list[6], 3), TOKENS // TOK)
    route_ids = jax.vmap(lambda own, number: deal_out(jax.random.fold_in(key_list[6], 2), own, number, TOK, EXPERTS, TOP, CAP, 1))(route_ids_keys, route_ids_turns).reshape((TOKENS, TOP))
    route_gates = jnp.clip(0.1 + 0.79999997 * jax.random.uniform(key_list[7], (TOKENS, TOP), jnp.float32) ** steps_of(key_list[7], (TOKENS, TOP), ((0, 4),), -0.2, 0.2), 0.1, 0.9)
    expert_gate = bell_draw(key_list[8], (EXPERTS, D, F), D ** -0.5, 0.09375, ((0, 4), (2, 8)))
    expert_up = bell_draw(key_list[9], (EXPERTS, D, F), D ** -0.5, 0.09375, ((0, 4), (2, 8)))
    expert_down = bell_draw(key_list[10], (EXPERTS, F, D), F ** -0.5, 0.125, ((0, 4), (1, 8)))
    cotangent = gaussian_with(key_list[11], (TOKENS, D), 1.0, 6.0, ((0, 4), (1, 8)), (0, 1, 8, 2.0))
    return {"moe_input": moe_input, "out_gate": out_gate, "in_gate": in_gate, "values": values, "conv_taps": conv_taps, "out_proj": out_proj, "route_ids": route_ids, "route_gates": route_gates, "expert_gate": expert_gate, "expert_up": expert_up, "expert_down": expert_down, "cotangent": cotangent}


def reference(moe_input, out_gate, in_gate, values, conv_taps, out_proj, route_ids, route_gates, expert_gate, expert_up, expert_down, cotangent):
    slots = N_SP * CAP
    flat_ids = route_ids.reshape(-1)
    owner = jnp.arange(TOKENS * TOP, dtype=jnp.int32) // TOP
    one_hot = (flat_ids[:, None] == jnp.arange(EXPERTS, dtype=jnp.int32)[None, :]).astype(jnp.int32)
    blocked = one_hot.reshape(N_SP, TOK * TOP, EXPERTS)
    earlier = (jnp.cumsum(blocked, axis=1) - blocked).reshape(TOKENS * TOP, EXPERTS)
    position = jnp.sum(earlier * one_hot, axis=1).astype(jnp.int32)
    slot_index = (flat_ids * slots + (owner // TOK) * CAP + position).astype(jnp.int32)
    slot_token = jnp.full((EXPERTS * slots,), TOKENS, jnp.int32).at[slot_index].set(owner)
    slot_weight = jnp.zeros((EXPERTS * slots,), jnp.float32).at[slot_index].set(route_gates.reshape(-1))
    padded_input = jnp.concatenate([moe_input, jnp.zeros((1, D), moe_input.dtype)], axis=0)
    padded_cot = jnp.concatenate([cotangent, jnp.zeros((1, D), cotangent.dtype)], axis=0)
    contract_rows = (((0,), (0,)), ((), ()))
    contract_cols = (((1,), (1,)), ((), ()))

    def expert_backward(args):
        tokens_of, weights_of, gate_w, up_w, down_w = args
        rows = padded_input[tokens_of]
        routed = (weights_of[:, None] * padded_cot[tokens_of].astype(jnp.float32)).astype(jnp.bfloat16)
        pre_gate = jnp.dot(rows, gate_w, preferred_element_type=jnp.float32)
        pre_up = jnp.dot(rows, up_w, preferred_element_type=jnp.float32)
        gate_sig = jax.nn.sigmoid(pre_gate)
        activated = pre_gate * gate_sig
        hidden_act = (activated * pre_up).astype(jnp.bfloat16)
        grad_down = lax.dot_general(hidden_act, routed, contract_rows, preferred_element_type=jnp.float32)
        grad_hidden = lax.dot_general(routed, down_w, contract_cols, preferred_element_type=jnp.float32)
        grad_pre_gate = (grad_hidden * pre_up * gate_sig * (1.0 + pre_gate * (1.0 - gate_sig))).astype(jnp.bfloat16)
        grad_pre_up = (grad_hidden * activated).astype(jnp.bfloat16)
        grad_gate = lax.dot_general(rows, grad_pre_gate, contract_rows, preferred_element_type=jnp.float32)
        grad_up = lax.dot_general(rows, grad_pre_up, contract_rows, preferred_element_type=jnp.float32)
        assign = (lax.dot_general(grad_pre_gate, gate_w, contract_cols, preferred_element_type=jnp.float32)
                  + lax.dot_general(grad_pre_up, up_w, contract_cols, preferred_element_type=jnp.float32))
        return grad_gate, grad_up, grad_down, assign

    grad_expert_gate, grad_expert_up, grad_expert_down, assign = lax.map(
        expert_backward,
        (slot_token.reshape(EXPERTS, slots), slot_weight.reshape(EXPERTS, slots), expert_gate, expert_up, expert_down))
    flat_assign = assign.reshape(EXPERTS * slots, D)
    moe_grad = jnp.sum(flat_assign[slot_index].reshape(TOKENS, TOP, D), axis=1)
    mixer_cot = (cotangent.astype(jnp.float32) + moe_grad).astype(jnp.bfloat16)

    conv_in = in_gate.astype(jnp.float32) * values.astype(jnp.float32)
    rimmed = jnp.pad(conv_in, ((1, 1), (0, 0)))
    conv_out = rimmed[:-2] * conv_taps[0] + rimmed[1:-1] * conv_taps[1] + rimmed[2:] * conv_taps[2]
    mixed = (out_gate.astype(jnp.float32) * conv_out).astype(jnp.bfloat16)
    grad_mixed = jnp.dot(mixer_cot, out_proj, preferred_element_type=jnp.float32)
    grad_out_gate = (grad_mixed * conv_out).astype(jnp.bfloat16)
    grad_conv_out = grad_mixed * out_gate.astype(jnp.float32)
    rim_grad = jnp.pad(grad_conv_out, ((1, 1), (0, 0)))
    grad_conv_in = rim_grad[2:] * conv_taps[0] + rim_grad[1:-1] * conv_taps[1] + rim_grad[:-2] * conv_taps[2]
    grad_in_gate = (grad_conv_in * values.astype(jnp.float32)).astype(jnp.bfloat16)
    grad_values = (grad_conv_in * in_gate.astype(jnp.float32)).astype(jnp.bfloat16)
    grad_out_proj = lax.dot_general(mixer_cot, mixed, contract_rows, preferred_element_type=jnp.float32)
    return (grad_out_gate, grad_in_gate, grad_values, grad_out_proj, grad_expert_gate, grad_expert_up, grad_expert_down)
```

```python
import jax
import jax.numpy as jnp
from jax import lax
from jax.experimental import pallas as pl
from jax.experimental.pallas import tpu as pltpu
from jax.sharding import PartitionSpec as P

MESH = pl.DeviceIdType.MESH


def peers_of(group):
    sp, tp = (lax.axis_index("sp"), lax.axis_index("tp"))
    if group == "core":
        me, size = (lax.rem(tp, 2), 2)
    elif group == "z":
        me, size = (lax.div(tp, 2), lax.axis_size("tp") // 2)
    else:
        me, size = (sp, lax.axis_size("sp"))
    others = []
    for k in range(1, size):
        place = lax.rem(me + k, size)
        if group == "core":
            others.append((place, (sp, tp - me + place)))
        elif group == "z":
            others.append((place, (sp, place * 2 + lax.rem(tp, 2))))
        else:
            others.append((place, (place, tp)))
    return me, others


def group_size(group):
    if group == "core":
        return 2
    return lax.axis_size("tp") // 2 if group == "z" else lax.axis_size("sp")


def block(ref, place, width):
    return ref.at[:, pl.ds(pl.multiple_of(place * width, width), width)]


def exchange(collective_id, *ops):
    arrays = [op[2] for op in ops]
    shapes = []
    counts = []
    for kind, group, array, *rest in ops:
        size = group_size(group)
        if kind == "cores":
            shape, count = ((array.shape[0], array.shape[1] // 2), array.shape[1] // rest[0] // 2)
        elif kind == "columns":
            shape = (size - 1, array.shape[0], array.shape[1] // size)
            count = size - 1
        elif kind == "rows":
            shape, count = ((size - 1,) + array.shape[1:], size - 1)
        elif kind == "gather":
            shape, count = ((array.shape[0], array.shape[1] * size), size - 1)
        elif kind == "send":
            shape, count = (array.shape, size - 1)
        else:
            shape, count = (array.shape, 1)
        shapes.append(jax.ShapeDtypeStruct(shape, array.dtype))
        counts.append(count)
    total = sum(counts)

    def kernel(*refs):
        n = len(ops)
        sources, targets = (refs[:n], refs[n : 2 * n])
        send_sem, recv_sem, own_sem = refs[2 * n :]
        barrier = pltpu.get_barrier_semaphore()
        greeted = 0
        for group in sorted({op[1] for op in ops}):
            for _, device in peers_of(group)[1]:
                pl.semaphore_signal(barrier, inc=1, device_id=device, device_id_type=MESH)
                greeted += 1
        pl.semaphore_wait(barrier, greeted)
        copies = []
        local = []
        for i, (kind, group, array, *rest) in enumerate(ops):
            me, others = peers_of(group)
            source, target = (sources[i], targets[i])
            moves = []
            if kind == "cores":
                width = rest[0]
                place, device = others[0]
                for b in range(counts[i]):
                    moves.append(
                        (
                            block(source, 2 * b + place, width),
                            target.at[:, pl.ds(b * width, width)],
                            device,
                        )
                    )
            for k, (place, device) in enumerate(others):
                if kind == "columns":
                    moves.append((block(source, place, shapes[i].shape[2]), target.at[k], device))
                elif kind == "rows":
                    moves.append((source.at[place], target.at[k], device))
                elif kind == "gather":
                    moves.append((source, block(target, me, array.shape[1]), device))
                elif kind == "send":
                    moves.append((source.at[place], target.at[me], device))
                elif kind == "swap":
                    moves.append((source, target, device))
            for a, b, device in moves:
                j = len(copies)
                copy = pltpu.make_async_remote_copy(
                    src_ref=a,
                    dst_ref=b,
                    send_sem=send_sem.at[j],
                    recv_sem=recv_sem.at[j],
                    device_id=device,
                    device_id_type=MESH,
                )
                copy.start()
                copies.append(copy)
            if kind == "gather":
                local.append((source, block(target, me, array.shape[1]), i))
            elif kind == "send":
                local.append((source.at[me], target.at[me], i))
        own = [pltpu.make_async_copy(a, b, own_sem.at[i]) for a, b, i in local]
        for copy in own:
            copy.start()
        for copy in own + copies:
            copy.wait()

    return pl.pallas_call(
        kernel,
        out_shape=shapes,
        in_specs=[pl.BlockSpec(memory_space=pl.ANY)] * len(ops),
        out_specs=[pl.BlockSpec(memory_space=pl.ANY)] * len(ops),
        scratch_shapes=[
            pltpu.SemaphoreType.DMA((total,)),
            pltpu.SemaphoreType.DMA((total,)),
            pltpu.SemaphoreType.DMA((len(ops),)),
        ],
        compiler_params=pltpu.CompilerParams(collective_id=collective_id, has_side_effects=True),
    )(*arrays)


def halves(array, width):
    rows, columns = array.shape
    split = array.reshape(rows, columns // width // 2, 2, width)
    core = lax.rem(lax.axis_index("tp"), 2)
    return jnp.where(core == 0, split[:, :, 0], split[:, :, 1]).reshape(rows, columns // 2)


def interleave(own, other, width):
    rows, columns = own.shape
    core = lax.rem(lax.axis_index("tp"), 2)
    own, other = (a.reshape(rows, columns // width, width) for a in (own, other))
    first, second = (jnp.where(core == 0, own, other), jnp.where(core == 0, other, own))
    return jnp.stack([first, second], axis=2).reshape(rows, 2 * columns)


def padded(array, sides, width):
    for axis, dim in sides:
        size, length = (lax.axis_size(axis), array.shape[dim])
        up = [(i, (i + 1) % size) for i in range(size - 1)]
        down = [(j, i) for i, j in up]
        last = lax.slice_in_dim(array, length - width, length, axis=dim)
        initial = lax.slice_in_dim(array, 0, width, axis=dim)
        before = lax.ppermute(last, axis, up)
        after = lax.ppermute(initial, axis, down)
        array = jnp.concatenate([before, array, after], axis=dim)
    return array


def body(
    moe_input,
    out_gate,
    in_gate,
    values,
    conv_taps,
    out_proj,
    route_ids,
    route_gates,
    expert_gate,
    expert_up,
    expert_down,
    cotangent,
):
    token_count = moe_input.shape[0]
    part_width = moe_input.shape[1]
    pick_count = route_ids.shape[1]
    group_count = lax.axis_size("sp")
    local_count = expert_gate.shape[0]
    expert_count = group_count * local_count
    capacity = 3 * token_count // expert_count
    contract_rows = (((0,), (0,)), ((), ()))
    flat_ids = route_ids.reshape(-1)
    owner = jnp.arange(token_count * pick_count, dtype=jnp.int32) // pick_count
    one_hot = (flat_ids[:, None] == jnp.arange(expert_count, dtype=jnp.int32)[None, :]).astype(
        jnp.int32
    )
    earlier = jnp.cumsum(one_hot, axis=0) - one_hot
    position = jnp.sum(earlier * one_hot, axis=1)
    slot_index = flat_ids * capacity + position
    slot_token = (
        jnp.full((expert_count * capacity,), token_count, jnp.int32).at[slot_index].set(owner)
    )
    slot_weight = (
        jnp.zeros((expert_count * capacity,), jnp.float32)
        .at[slot_index]
        .set(route_gates.reshape(-1))
    )
    padded_input = jnp.concatenate([moe_input, jnp.zeros((1, part_width), moe_input.dtype)], axis=0)
    padded_cot = jnp.concatenate([cotangent, jnp.zeros((1, part_width), cotangent.dtype)], axis=0)
    send_rows = padded_input[slot_token].reshape(expert_count, capacity, part_width)
    send_cot = (slot_weight[:, None] * padded_cot[slot_token].astype(jnp.float32)).astype(
        jnp.bfloat16
    )
    send_cot = send_cot.reshape(expert_count, capacity, part_width)
    recv_rows, recv_cot = (
        lax.all_to_all(send_rows, "sp", split_axis=0, concat_axis=1, tiled=True),
        lax.all_to_all(send_cot, "sp", split_axis=0, concat_axis=1, tiled=True),
    )
    full_rows, full_cot = (
        lax.all_gather(recv_rows, "tp", axis=2, tiled=True),
        lax.all_gather(recv_cot, "tp", axis=2, tiled=True),
    )
    pre_gate = jnp.einsum(
        "prd,pdf->prf", full_rows, expert_gate, preferred_element_type=jnp.float32
    )
    pre_up = jnp.einsum("prd,pdf->prf", full_rows, expert_up, preferred_element_type=jnp.float32)
    gate_sig = jax.nn.sigmoid(pre_gate)
    activated = pre_gate * gate_sig
    hidden_act = (activated * pre_up).astype(jnp.bfloat16)
    grad_expert_down = jnp.einsum(
        "prf,prd->pfd", hidden_act, full_cot, preferred_element_type=jnp.float32
    )
    grad_hidden = jnp.einsum(
        "prd,pfd->prf", full_cot, expert_down, preferred_element_type=jnp.float32
    )
    grad_pre_gate = (grad_hidden * pre_up * gate_sig * (1.0 + pre_gate * (1.0 - gate_sig))).astype(
        jnp.bfloat16
    )
    grad_pre_up = (grad_hidden * activated).astype(jnp.bfloat16)
    grad_expert_gate = jnp.einsum(
        "prd,prf->pdf", full_rows, grad_pre_gate, preferred_element_type=jnp.float32
    )
    grad_expert_up = jnp.einsum(
        "prd,prf->pdf", full_rows, grad_pre_up, preferred_element_type=jnp.float32
    )
    partial_grad = jnp.einsum(
        "prf,pdf->prd", grad_pre_gate, expert_gate, preferred_element_type=jnp.float32
    ) + jnp.einsum("prf,pdf->prd", grad_pre_up, expert_up, preferred_element_type=jnp.float32)
    me = lax.axis_index("sp")
    block_rows = local_count * capacity
    partial_rows = partial_grad.astype(jnp.bfloat16).reshape(local_count * group_count * capacity, -1)
    (other_core,) = exchange(1, ("cores", "core", partial_rows, part_width))
    chip_rows = (
        halves(partial_rows, part_width).astype(jnp.float32) + other_core.astype(jnp.float32)
    ).astype(jnp.bfloat16)
    half = chip_rows.shape[1]
    chip_rows = jnp.swapaxes(
        chip_rows.reshape(local_count, group_count, capacity, half), 0, 1
    ).reshape(group_count, block_rows, half)
    (returned,) = exchange(2, ("rows", "sp", chip_rows))
    back = lax.rem(me - jnp.arange(group_count) + group_count, group_count)
    local_slots = jnp.arange(block_rows, dtype=jnp.int32)
    picks = jnp.sum(
        (slot_index.reshape(token_count, pick_count)[None, :, :, None])
        == (back[:, None] * block_rows + local_slots)[:, None, None, :],
        axis=2,
    ).astype(jnp.bfloat16)
    token_part = jnp.dot(
        picks[0],
        lax.dynamic_index_in_dim(chip_rows, me, 0, keepdims=False),
        preferred_element_type=jnp.float32,
    ) + jnp.einsum("kts,ksd->td", picks[1:], returned, preferred_element_type=jnp.float32)
    token_part = token_part.astype(jnp.bfloat16)
    (parts,) = exchange(3, ("columns", "z", token_part))
    own_part = lax.dynamic_slice_in_dim(
        token_part, lax.div(lax.axis_index("tp"), 2) * part_width, part_width, axis=1
    )
    moe_grad = own_part.astype(jnp.float32) + jnp.sum(parts.astype(jnp.float32), axis=0)
    mixer_cot = (cotangent.astype(jnp.float32) + moe_grad).astype(jnp.bfloat16)
    conv_in = in_gate.astype(jnp.float32) * values.astype(jnp.float32)
    rimmed = padded(conv_in, (("sp", 0),), 1)
    conv_out = rimmed[:-2] * conv_taps[0] + rimmed[1:-1] * conv_taps[1] + rimmed[2:] * conv_taps[2]
    mixed = (out_gate.astype(jnp.float32) * conv_out).astype(jnp.bfloat16)
    full_mixer_cot = lax.all_gather(mixer_cot, "tp", axis=1, tiled=True)
    grad_mixed = jnp.dot(full_mixer_cot, out_proj, preferred_element_type=jnp.float32)
    grad_out_gate = (grad_mixed * conv_out).astype(jnp.bfloat16)
    grad_conv_out = grad_mixed * out_gate.astype(jnp.float32)
    rim_grad = padded(grad_conv_out, (("sp", 0),), 1)
    grad_conv_in = (
        rim_grad[2:] * conv_taps[0] + rim_grad[1:-1] * conv_taps[1] + rim_grad[:-2] * conv_taps[2]
    )
    grad_in_gate = (grad_conv_in * values.astype(jnp.float32)).astype(jnp.bfloat16)
    grad_values = (grad_conv_in * in_gate.astype(jnp.float32)).astype(jnp.bfloat16)
    columns = lax.all_to_all(full_mixer_cot, "sp", split_axis=1, concat_axis=0, tiled=True)
    grad_out_proj = lax.dot_general(
        columns,
        lax.all_gather(mixed, "sp", axis=0, tiled=True),
        contract_rows,
        preferred_element_type=jnp.float32,
    )
    return (
        grad_out_gate,
        grad_in_gate,
        grad_values,
        grad_out_proj,
        grad_expert_gate,
        grad_expert_up,
        grad_expert_down,
    )


def solution(mesh):
    return jax.shard_map(
        body,
        mesh=mesh,
        in_specs=(
            P("sp", "tp"),
            P("sp", "tp"),
            P("sp", "tp"),
            P("sp", "tp"),
            P(None, "tp"),
            P(None, "tp"),
            P("sp", None),
            P("sp", None),
            P("sp", None, "tp"),
            P("sp", None, "tp"),
            P("sp", "tp", None),
            P("sp", "tp"),
        ),
        out_specs=(
            P("sp", "tp"),
            P("sp", "tp"),
            P("sp", "tp"),
            P("sp", "tp"),
            P("sp", None, "tp"),
            P("sp", None, "tp"),
            P("sp", "tp", None),
        ),
        check_vma=False,
    )
```
